32 devices in a mesh: sp: 8 (over z, x), dp: 4 (over y, core).
Axes of the slice: x: 2, y: 2, z: 4, core: 2. Of those that a mesh axis runs over, the one named last changes fastest.
Arguments:
- residual: bfloat16 [4, 1024, 2048], P('dp', 'sp'), may hold values from -6 to 6
- query: bfloat16 [4, 1024, 2048], P('dp', 'sp'), may hold values from -6 to 6
- key: bfloat16 [4, 1024, 2048], P('dp', 'sp'), may hold values from -6 to 6
- value: bfloat16 [4, 1024, 2048], P('dp', 'sp'), may hold values from -6 to 6
- output_gate_input: bfloat16 [4, 1024, 2048], P('dp', 'sp'), may hold values from -6 to 6
- write_strength_logit: bfloat16 [4, 1024, 16], P('dp', 'sp'), may hold values from -6 to 6
- decay_head_input: bfloat16 [4, 1024, 16], P('dp', 'sp'), may hold values from -5 to 5
- added_log_decay: float32 [4, 16, 1024], P('dp', 'sp'), may hold values from -2 to 0
- head_decay_rate: float32 [16], P('sp'), may hold values from 0 to 1
- head_norm_gain: float32 [128], replicated, may hold values from 0.1 to 1.9
- output_projection: bfloat16 [2048, 2048], P(None, 'dp'), may hold values from -0.125 to 0.125
- mixer_norm_gain: float32 [2048], replicated, may hold values from 0.1 to 1.9
- token_expert_index: int32 [4, 1024, 4], P('dp', 'sp'), may hold values from 0 to 31, all different within a row; in each aligned block of 128 rows (0 to 127, 128 to 255, ..., all dimensions but the last counted through in order) at most 24 rows name the same one
- token_expert_weight: float32 [4, 1024, 4], P('dp', 'sp'), may hold values from 0.1 to 0.6
- expert_gate_weight: bfloat16 [32, 2048, 1024], P(('sp', 'dp')), may hold values from -1 to 1
- expert_up_weight: bfloat16 [32, 2048, 1024], P(('sp', 'dp')), may hold values from -1 to 1
- expert_down_weight: bfloat16 [32, 1024, 2048], P(('sp', 'dp')), may hold values from -0.1875 to 0.1875
- feedforward_norm_gain: float32 [2048], replicated, may hold values from 0.1 to 1.9
Outputs:
- blended: float32 [4, 1024, 2048], P('dp', 'sp')
The draws below stay inside these ranges and needn't reach their ends.
Inputs may be any that keep to these rules, and one draw needn't show every extreme that they name: `token_expert_index`: each row names 4 different experts; within the 128 rows of one device no expert is named by more than 24 rows, and in every draw some expert is named by exactly 24 rows of some device.
All inputs are finite; a program needn't handle non-finite values.
Results may differ from the reference program's by a relative error of at most 0.0062.
Values may be sent and summed in bfloat16 or wider, within the bound.
A program may use at most 128 MiB of HBM per device.

```python
import math
import jax
import jax.numpy as jnp
import numpy as np
from jax import lax

D = 2048
RECURRENT_HEADS = 16
HD = 128
WIDTH = 2048
FF = 1024
TOP = 4
SPAN = 64
TOK_DEV = 128
SEQUENCE_COUNT = 4
SEQUENCE_LENGTH = 1024
EXPERTS = 32
CAP = 24


def draw_decay_head_input(key, part):
    base_key = jax.random.fold_in(key, 21)
    noise_key, level_key = jax.random.split(base_key)
    noise = jax.random.normal(noise_key, (SEQUENCE_COUNT, SEQUENCE_LENGTH, RECURRENT_HEADS), jnp.float32)
    levels = jax.random.uniform(level_key, (SEQUENCE_COUNT, SEQUENCE_LENGTH // TOK_DEV, 1, RECURRENT_HEADS), jnp.float32, -1.0, 1.5)
    levels = jnp.broadcast_to(levels, (SEQUENCE_COUNT, SEQUENCE_LENGTH // TOK_DEV, TOK_DEV, RECURRENT_HEADS)).reshape(SEQUENCE_COUNT, SEQUENCE_LENGTH, RECURRENT_HEADS)
    return jnp.clip(noise + levels, -5.0, 5.0).astype(jnp.bfloat16)


def draw_added_log_decay(key, part):
    base_key = jax.random.fold_in(key, 22)
    where_key, kept_key = jax.random.split(base_key)
    spots = jax.random.randint(where_key, (SEQUENCE_COUNT, RECURRENT_HEADS, 2, 1), 0, SEQUENCE_LENGTH)
    kept = jax.random.uniform(kept_key, (SEQUENCE_COUNT, RECURRENT_HEADS, 2, 1), jnp.float32, 0.5, 0.8)
    places = jnp.arange(SEQUENCE_LENGTH)[None, None, None, :]
    return jnp.sum(jnp.where(places == spots, jnp.log(kept), 0.0), axis=2).astype(jnp.float32)


def draw_head_decay_rate(key, part):
    base_key = jax.random.fold_in(key, 23)
    order_key, fast_key, slow_key = jax.random.split(base_key, 3)
    ranks = jax.random.permutation(order_key, RECURRENT_HEADS)
    fast = jax.random.uniform(fast_key, (RECURRENT_HEADS,), jnp.float32, 0.02, 0.05)
    slow = jax.random.uniform(slow_key, (RECURRENT_HEADS,), jnp.float32, 0.1, 0.3) / SEQUENCE_LENGTH
    return jnp.where(ranks < RECURRENT_HEADS // 2, fast, slow)


def expert_input_weight(key):
    entry_key = jax.random.fold_in(key, 0)
    entries = jax.random.normal(entry_key, (EXPERTS, D, FF), jnp.float32) / math.sqrt(D)
    return jnp.clip(entries, -1.0, 1.0).astype(jnp.bfloat16)


def draw_expert_gate_weight(key, part):
    return expert_input_weight(jax.random.fold_in(key, 11))


def draw_expert_up_weight(key, part):
    return expert_input_weight(jax.random.fold_in(key, 12))


def shard_levels(own_key, dims, cuts, smallest, top_value):
    loudness, own = 1.0, jax.random.fold_in(own_key, 6)
    for axis_at, blocks in cuts:
        draws = jnp.exp(jax.random.uniform(jax.random.fold_in(own, axis_at), (blocks,), jnp.float32, smallest / len(cuts), top_value / len(cuts)))
        loudness = loudness * jnp.repeat(draws, dims[axis_at] // blocks).reshape([-1 if axis == axis_at else 1 for axis in range(len(dims))])
    return loudness


def shared_out(stream_key, own, number, rows, amount, top, reach, lean):
    sequence = jax.random.permutation(stream_key, amount)
    packed, usual = shares(amount, rows * top, reach, lean, True), shares(amount, rows * top, reach, lean, False)
    places = jnp.arange(amount)

    def named(tallies, offset_by):
        used = int((tallies > 0).sum())
        fixed = max(1, used // 4)
        moved = fixed + (places - fixed + offset_by * (used - fixed)) % max(1, amount - fixed)
        return jnp.zeros((amount,), jnp.int32).at[sequence[jnp.where(places < fixed, places, moved)]].set(jnp.asarray(tallies, jnp.int32))

    tallies = jnp.where(number % 4 == 0, named(packed, number // 4), named(usual, number - number // 4 - 1))
    mixed = jax.random.permutation(jax.random.fold_in(own, 3), amount)
    giver, sink = mixed[0:amount // 2 * 2:2], mixed[1:amount // 2 * 2:2]
    room = jnp.minimum(tallies[giver] - 1, reach - tallies[sink]) // 2
    room = jnp.where((giver == sequence[0]) | (sink == sequence[0]) | (tallies[sink] == 0), 0, jnp.maximum(room, 0))
    moved = jax.random.randint(jax.random.fold_in(own, 4), (amount // 2,), 0, 1 << 20) % (room + 1)
    tallies = tallies.at[giver].add(-moved).at[sink].add(moved)
    items = jnp.searchsorted(jnp.cumsum(tallies), jnp.arange(rows * top), side="right").astype(jnp.int32)
    listing = items.reshape(top, rows).T
    listing = listing[jax.random.permutation(jax.random.fold_in(own, 1), rows)]
    offset_by = jax.random.randint(jax.random.fold_in(own, 2), (rows, 1), 0, top)
    return jnp.take_along_axis(listing, (jnp.arange(top)[None, :] + offset_by) % top, axis=1)


def shares(count, total, bound, slope, full):
    loads = [(1 << 20) // math.isqrt(grade ** slope) + 1 for grade in range(1, count + 1)]
    largest = bound if full else min(bound, max(-(-total // count), total * loads[0] // sum(loads)))
    least = 1 if total - largest >= count - 1 else 0
    holding, rest = [largest] + [least] * (count - 1), total - largest - least * (count - 1)
    while rest > 0:
        free = [i for i in range(1, count) if holding[i] < largest] or [i for i in range(1, count) if holding[i] < bound]
        pool, left = sum([loads[i] for i in free]), rest
        for i in free:
            extra = min(bound - holding[i], max(1, left * loads[i] // pool), rest)
            holding[i] = holding[i] + extra
            rest = rest - extra
    return np.array(holding)


def bell_draw(own_key, dims, spread, reach, shards=(), held_as=jnp.bfloat16):
    drawn = spread * jax.random.normal(own_key, dims, jnp.float32)
    if shards:
        drawn = drawn * shard_levels(own_key, dims, shards, -0.22, 0.18)
    return jnp.clip(drawn, -reach, reach).astype(held_as)


def setup_inputs(seed: int = 0) -> dict:
    keys = jax.random.split(jax.random.key(seed), 19)
    residual = bell_draw(keys[0], (SEQUENCE_COUNT, SEQUENCE_LENGTH, D), 1.0, 6.0, ((0, 4), (1, 8)))
    query = bell_draw(keys[1], (SEQUENCE_COUNT, SEQUENCE_LENGTH, WIDTH), 1.0, 6.0, ((0, 4), (1, 8)))
    key = bell_draw(keys[2], (SEQUENCE_COUNT, SEQUENCE_LENGTH, WIDTH), 1.0, 6.0, ((0, 4), (1, 8)))
    value = bell_draw(keys[3], (SEQUENCE_COUNT, SEQUENCE_LENGTH, WIDTH), 1.0, 6.0, ((0, 4), (1, 8)))
    output_gate_input = bell_draw(keys[4], (SEQUENCE_COUNT, SEQUENCE_LENGTH, WIDTH), 1.0, 6.0, ((0, 4), (1, 8)))
    write_strength_logit = bell_draw(keys[5], (SEQUENCE_COUNT, SEQUENCE_LENGTH, RECURRENT_HEADS), 1.5, 6.0, ((0, 4), (1, 8)))
    decay_head_input = draw_decay_head_input(jax.random.fold_in(keys[18], 71), 0)
    added_log_decay = draw_added_log_decay(jax.random.fold_in(keys[18], 71), 0)
    head_decay_rate = draw_head_decay_rate(jax.random.fold_in(keys[18], 71), 0)
    head_norm_gain = jnp.clip(1.0 + 0.18 * jax.random.normal(keys[9], (HD,), jnp.float32), 0.1, 1.9)
    output_projection = bell_draw(keys[10], (WIDTH, D), WIDTH ** -0.5, 0.125, ((1, 4),))
    mixer_norm_gain = jnp.clip(1.0 + 0.18 * jax.random.normal(keys[11], (D,), jnp.float32), 0.1, 1.9)
    token_expert_index_keys = jax.random.split(jax.random.fold_in(keys[12], 1), SEQUENCE_COUNT * SEQUENCE_LENGTH // TOK_DEV)
    token_expert_index_turns = jax.random.permutation(jax.random.fold_in(keys[12], 3), SEQUENCE_COUNT * SEQUENCE_LENGTH // TOK_DEV)
    token_expert_index = jax.vmap(lambda own, number: shared_out(jax.random.fold_in(keys[12], 2), own, number, TOK_DEV, EXPERTS, TOP, CAP, 2))(token_expert_index_keys, token_expert_index_turns).reshape((SEQUENCE_COUNT, SEQUENCE_LENGTH, TOP))
    token_expert_weight = jnp.clip(0.1 + 0.5 * jax.random.uniform(keys[13], (SEQUENCE_COUNT, SEQUENCE_LENGTH, TOP), jnp.float32) ** shard_levels(keys[13], (SEQUENCE_COUNT, SEQUENCE_LENGTH, TOP), ((0, 4), (1, 8)), -0.2, 0.2), 0.1, 0.6)
    expert_gate_weight = draw_expert_gate_weight(jax.random.fold_in(keys[18], 71), 0)
    expert_up_weight = draw_expert_up_weight(jax.random.fold_in(keys[18], 71), 0)
    expert_down_weight = bell_draw(keys[16], (EXPERTS, FF, D), FF ** -0.5, 0.1875, ((0, 32),))
    feedforward_norm_gain = jnp.clip(1.0 + 0.18 * jax.random.normal(keys[17], (D,), jnp.float32), 0.1, 1.9)
    return {"residual": residual, "query": query, "key": key, "value": value, "output_gate_input": output_gate_input, "write_strength_logit": write_strength_logit, "decay_head_input": decay_head_input, "added_log_decay": added_log_decay, "head_decay_rate": head_decay_rate, "head_norm_gain": head_norm_gain, "output_projection": output_projection, "mixer_norm_gain": mixer_norm_gain, "token_expert_index": token_expert_index, "token_expert_weight": token_expert_weight, "expert_gate_weight": expert_gate_weight, "expert_up_weight": expert_up_weight, "expert_down_weight": expert_down_weight, "feedforward_norm_gain": feedforward_norm_gain}


HIGHEST = lax.Precision.HIGHEST
CLAMP_LIMIT = 7.0
SWISH_SLOPE = 1.702

def unit_lower_inverse(strict_part):
    order_len = strict_part.shape[-1]
    identity = jnp.eye(order_len, dtype=jnp.float32)
    result = identity - strict_part
    squared = strict_part
    for _unused in range(int(math.log2(order_len)) - 1):
        squared = jnp.einsum('nij,njk->nik', squared, squared, precision=HIGHEST)
        result = jnp.einsum('nij,njk->nik', result, identity + squared, precision=HIGHEST)
    return result

def delta_rule(q_unit, k_unit, values, write_rate, log_decay):
    length, head_dim = q_unit.shape
    blocks = length // SPAN
    q_block = q_unit.reshape(blocks, SPAN, head_dim)
    k_block = k_unit.reshape(blocks, SPAN, head_dim)
    v_block = values.reshape(blocks, SPAN, head_dim)
    rate_block = write_rate.reshape(blocks, SPAN)
    cumulative = jnp.cumsum(log_decay.reshape(blocks, SPAN), axis=1)
    position = jnp.arange(SPAN)
    strict = position[:, None] > position[None, :]
    inclusive = position[:, None] >= position[None, :]
    within = jnp.exp(jnp.where(inclusive, cumulative[:, :, None] - cumulative[:, None, :], -jnp.inf))
    keys_dot = jnp.einsum('nid,njd->nij', k_block, k_block, precision=HIGHEST)
    lower_part = jnp.where(strict, rate_block[:, :, None] * within * keys_dot, 0.0)
    inverse = unit_lower_inverse(lower_part)
    right_side = jnp.concatenate([rate_block[..., None] * v_block, (rate_block * jnp.exp(cumulative))[..., None] * k_block], axis=-1)
    solved = jnp.einsum('nij,njd->nid', inverse, right_side, precision=HIGHEST)
    base_part = solved[..., :head_dim]
    weight_part = solved[..., head_dim:]
    scores = jnp.einsum('nid,njd->nij', q_block, k_block, precision=HIGHEST) * within
    q_decayed = q_block * jnp.exp(cumulative)[..., None]
    k_decayed = k_block * jnp.exp(cumulative[:, -1:] - cumulative)[..., None]
    carried = jnp.exp(cumulative[:, -1])

    def advance(state, inputs):
        base_rows, weight_rows, score_rows, q_rows, k_rows, carry_rate = inputs
        fresh = base_rows - jnp.dot(weight_rows, state, precision=HIGHEST)
        output = jnp.dot(q_rows, state, precision=HIGHEST) + jnp.dot(score_rows, fresh, precision=HIGHEST)
        state = state * carry_rate + jnp.dot(k_rows.T, fresh, precision=HIGHEST)
        return (state, output)
    initial = jnp.zeros((head_dim, head_dim), jnp.float32)
    _, outputs = lax.scan(advance, initial, (base_part, weight_part, scores, q_decayed, k_decayed, carried))
    return outputs.reshape(length, head_dim)

def unit_rows(values):
    values = values.astype(jnp.float32)
    return values * lax.rsqrt(lax.optimization_barrier(jnp.sum(values * values, -1, keepdims=True)) + 1e-06)

def head_output(recurrent, gate_input, head_norm_gain):
    norm_scale = lax.rsqrt(lax.optimization_barrier(jnp.mean(recurrent * recurrent, -1, keepdims=True)) + 1e-05)
    return (recurrent * norm_scale * head_norm_gain * jax.nn.silu(gate_input.astype(jnp.float32))).astype(jnp.bfloat16)

def layer_norm(values, gain):
    average = lax.optimization_barrier(jnp.mean(values, -1, keepdims=True))
    centred = values - average
    variance = lax.optimization_barrier(jnp.mean(centred * centred, -1, keepdims=True))
    return centred * lax.rsqrt(variance + 1e-05) * gain

def expert_rows(rows, gate_weight, up_weight, down_weight):
    gate = jnp.minimum(jnp.dot(rows, gate_weight, preferred_element_type=jnp.float32), CLAMP_LIMIT)
    upper = jnp.clip(jnp.dot(rows, up_weight, preferred_element_type=jnp.float32), -CLAMP_LIMIT, CLAMP_LIMIT)
    hidden = (gate * jax.nn.sigmoid(SWISH_SLOPE * gate) * (upper + 1.0)).astype(jnp.bfloat16)
    return jnp.dot(hidden, down_weight, preferred_element_type=jnp.float32).astype(jnp.bfloat16)

def reference(residual, query, key, value, output_gate_input, write_strength_logit, decay_head_input, added_log_decay, head_decay_rate, head_norm_gain, output_projection, mixer_norm_gain, token_expert_index, token_expert_weight, expert_gate_weight, expert_up_weight, expert_down_weight, feedforward_norm_gain):

    def by_head(values):
        return values.reshape(SEQUENCE_COUNT, SEQUENCE_LENGTH, RECURRENT_HEADS, HD).transpose(0, 2, 1, 3).reshape(SEQUENCE_COUNT * RECURRENT_HEADS, SEQUENCE_LENGTH, HD)
    q_heads = by_head(query)
    k_heads = by_head(key)
    v_heads = by_head(value)
    rate_heads = jax.nn.sigmoid(write_strength_logit.astype(jnp.float32)).transpose(0, 2, 1).reshape(SEQUENCE_COUNT * RECURRENT_HEADS, SEQUENCE_LENGTH)
    head_decays = (-head_decay_rate[None, :, None] * jax.nn.softplus(decay_head_input.astype(jnp.float32).transpose(0, 2, 1)) + added_log_decay).reshape(SEQUENCE_COUNT * RECURRENT_HEADS, SEQUENCE_LENGTH)

    def one_head(index):
        return delta_rule(unit_rows(q_heads[index]) * HD ** (-0.5), unit_rows(k_heads[index]), v_heads[index].astype(jnp.float32), rate_heads[index], head_decays[index])
    recurrent = lax.map(one_head, jnp.arange(SEQUENCE_COUNT * RECURRENT_HEADS))
    recurrent = recurrent.reshape(SEQUENCE_COUNT, RECURRENT_HEADS, SEQUENCE_LENGTH, HD).transpose(0, 2, 1, 3)
    gated = head_output(recurrent, output_gate_input.reshape(SEQUENCE_COUNT, SEQUENCE_LENGTH, RECURRENT_HEADS, HD), head_norm_gain)
    gated = gated.reshape(SEQUENCE_COUNT * SEQUENCE_LENGTH, WIDTH)
    mixed = jnp.dot(gated, output_projection, preferred_element_type=jnp.float32)
    normed = layer_norm(residual.reshape(SEQUENCE_COUNT * SEQUENCE_LENGTH, D).astype(jnp.float32) + mixed, mixer_norm_gain).astype(jnp.bfloat16)
    tokens = SEQUENCE_COUNT * SEQUENCE_LENGTH
    flat_ids = token_expert_index.reshape(-1)
    flat_weight = jnp.concatenate([token_expert_weight.reshape(-1), jnp.zeros((1,), jnp.float32)])
    padded = jnp.concatenate([normed, jnp.zeros((1, D), jnp.bfloat16)], 0)

    def one_expert(total, expert):
        chosen = jnp.nonzero(flat_ids == expert, size=EXPERTS * CAP, fill_value=tokens * TOP)[0]
        token_index = (chosen // TOP).astype(jnp.int32)
        weight = flat_weight[chosen]
        produced = expert_rows(padded[token_index], expert_gate_weight[expert], expert_up_weight[expert], expert_down_weight[expert])
        return (total.at[token_index].add(weight[:, None] * produced.astype(jnp.float32)), None)
    moe, _ = lax.scan(one_expert, jnp.zeros((tokens + 1, D), jnp.float32), jnp.arange(EXPERTS))
    blended = layer_norm(normed.astype(jnp.float32) + moe[:tokens], feedforward_norm_gain)
    return blended.reshape(SEQUENCE_COUNT, SEQUENCE_LENGTH, D)
```

```python
import functools

import jax
import jax.numpy as jnp
from jax import lax
from jax.experimental import pallas as pl
from jax.experimental.pallas import tpu as pltpu
from jax.sharding import PartitionSpec as P

CLAMP_LIMIT = 7.0
SWISH_SLOPE = 1.702
MESH = pl.DeviceIdType.MESH


def greet_peers(count):
    me = lax.axis_index("sp")
    barrier = pltpu.get_barrier_semaphore()
    for offset in range(1, count):
        pl.semaphore_signal(
            barrier, inc=1, device_id={"sp": lax.rem(me + offset, count)}, device_id_type=MESH
        )
    pl.semaphore_wait(barrier, count - 1)


def spread_heads_kernel(count, *refs):
    arrays = (len(refs) - 3) // 2
    sources, targets = refs[:arrays], refs[arrays : 2 * arrays]
    send_sem, recv_sem, local_sem = refs[2 * arrays :]
    me = lax.axis_index("sp")

    def piece(source, owner):
        if source.shape[0] == count:
            return source.at[owner]
        width = source.shape[2] // count
        return source.at[0, :, pl.ds(pl.multiple_of(owner * width, width), width)]

    def place(target, owner):
        return target.at[owner]

    greet_peers(count)
    copies = []
    for offset in range(1, count):
        peer = lax.rem(me + offset, count)
        for at in range(arrays):
            copy = pltpu.make_async_remote_copy(
                src_ref=piece(sources[at], peer),
                dst_ref=place(targets[at], me),
                send_sem=send_sem.at[at, offset],
                recv_sem=recv_sem.at[at, offset],
                device_id={"sp": peer},
                device_id_type=MESH,
            )
            copy.start()
            copies.append(copy)
    for at in range(arrays):
        copy = pltpu.make_async_copy(
            piece(sources[at], me), place(targets[at], me), local_sem.at[at]
        )
        copy.start()
        copies.append(copy)
    for copy in copies:
        copy.wait()


def spread_heads(sources, count):
    shapes = []
    for source in sources:
        if source.shape[0] == count:
            shapes.append(jax.ShapeDtypeStruct(source.shape, source.dtype))
        else:
            shapes.append(
                jax.ShapeDtypeStruct(
                    (count, source.shape[1], source.shape[2] // count), source.dtype
                )
            )
    return pl.pallas_call(
        functools.partial(spread_heads_kernel, count),
        out_shape=shapes,
        in_specs=[pl.BlockSpec(memory_space=pltpu.VMEM)] * len(sources),
        out_specs=[pl.BlockSpec(memory_space=pl.ANY)] * len(sources),
        scratch_shapes=[
            pltpu.SemaphoreType.DMA((len(sources), count)),
            pltpu.SemaphoreType.DMA((len(sources), count)),
            pltpu.SemaphoreType.DMA((len(sources),)),
        ],
        compiler_params=pltpu.CompilerParams(collective_id=0, has_side_effects=True),
    )(*sources)


def return_rows_kernel(count, source, target, send_sem, recv_sem, local_sem):
    me = lax.axis_index("sp")
    width = source.shape[2]
    own_columns = pl.ds(pl.multiple_of(me * width, width), width)
    greet_peers(count)
    copies = []
    for offset in range(1, count):
        peer = lax.rem(me + offset, count)
        copy = pltpu.make_async_remote_copy(
            src_ref=source.at[peer],
            dst_ref=target.at[:, own_columns],
            send_sem=send_sem.at[offset],
            recv_sem=recv_sem.at[offset],
            device_id={"sp": peer},
            device_id_type=MESH,
        )
        copy.start()
        copies.append(copy)
    copy = pltpu.make_async_copy(source.at[me], target.at[:, own_columns], local_sem)
    copy.start()
    copies.append(copy)
    for copy in copies:
        copy.wait()


def return_rows(source, count):
    return pl.pallas_call(
        functools.partial(return_rows_kernel, count),
        out_shape=jax.ShapeDtypeStruct(
            (source.shape[1], source.shape[2] * count), source.dtype
        ),
        in_specs=[pl.BlockSpec(memory_space=pltpu.VMEM)],
        out_specs=pl.BlockSpec(memory_space=pltpu.VMEM),
        scratch_shapes=[
            pltpu.SemaphoreType.DMA((count,)),
            pltpu.SemaphoreType.DMA((count,)),
            pltpu.SemaphoreType.DMA,
        ],
        compiler_params=pltpu.CompilerParams(collective_id=1, has_side_effects=True),
    )(source)


def dot(left, right):
    return jnp.dot(left, right, preferred_element_type=jnp.float32)


def halves(values):
    high = values.astype(jnp.bfloat16)
    return high, (values - high.astype(jnp.float32)).astype(jnp.bfloat16)


def dot3(left, right):
    return dot(left[0], right[0]) + (dot(left[0], right[1]) + dot(left[1], right[0]))


def rows_by_rows(left, right):
    return lax.dot_general(
        left, right, (((1,), (1,)), ((), ())), preferred_element_type=jnp.float32
    )


def recurrence_kernel(
    q_ref, k_ref, v_ref, small_ref, added_ref, decay_ref, gain_ref, out_ref,
    base_ref, weight_high, weight_low, score_ref, column_ref, state_ref,
):
    blocks, span, width = q_ref.shape
    heads = added_ref.shape[1]
    head_dim = width // heads
    row = lax.broadcasted_iota(jnp.int32, (span, span), 0)
    column = lax.broadcasted_iota(jnp.int32, (span, span), 1)
    same = row == column
    inclusive = row >= column
    strict = row > column
    identity = same.astype(jnp.float32)

    def to_column(values):
        return jnp.sum(jnp.where(same, values, 0.0), axis=1, keepdims=True)

    def to_row(values):
        return jnp.sum(jnp.where(same, values, 0.0), axis=0, keepdims=True)

    lanes = lax.broadcasted_iota(jnp.int32, (span, head_dim), 1)
    together = 2 if blocks % 2 == 0 else 1

    def prepare(step, carry):
        chains = [(step * together + i, h) for i in range(together) for h in range(heads)]
        lowers = []
        kept = []
        for block, head in chains:
            columns = slice(head * head_dim, (head + 1) * head_dim)
            q_raw = q_ref[block, :, columns]
            k_raw = k_ref[block, :, columns]
            q_wide = q_raw.astype(jnp.float32)
            q_rate = (
                lax.rsqrt(jnp.sum(q_wide * q_wide, 1, keepdims=True) + 1e-06)
                * head_dim ** (-0.5)
            )
            k_dot = rows_by_rows(k_raw, k_raw)
            k_wide = k_raw.astype(jnp.float32)
            k_rate = lax.rsqrt(jnp.sum(k_wide * k_wide, 1, keepdims=True) + 1e-06)
            k_rate_row = to_row(k_rate)
            rate_row = jax.nn.sigmoid(small_ref[block, head : head + 1, :])
            sequence_row = small_ref[block, heads + head : heads + head + 1, :]
            softplus = jnp.maximum(sequence_row, 0.0) + jnp.log1p(
                jnp.exp(-jnp.abs(sequence_row))
            )
            log_decay = (
                added_ref[block, head : head + 1, :] - decay_ref[head] * softplus
            )
            total = jnp.sum(jnp.where(inclusive, log_decay, 0.0), axis=1, keepdims=True)
            total_row = to_row(total)
            last = total[span - 1 : span, :]
            within = jnp.exp(jnp.where(inclusive, total - total_row, -1e30))
            lower = jnp.where(
                strict, to_column(rate_row) * within * k_dot * (k_rate * k_rate_row), 0.0
            )
            scores = rows_by_rows(q_raw, k_raw) * within * (q_rate * k_rate_row)
            rows = pl.ds(pl.multiple_of(block * span, span), span)
            score_ref[head, rows, :] = scores.astype(jnp.bfloat16)
            column_ref[head, rows, :] = jnp.where(
                lanes == 0,
                q_rate * jnp.exp(total),
                jnp.where(lanes == 1, k_rate * jnp.exp(last - total), jnp.exp(last)),
            )
            lowers.append(lower)
            kept.append((rate_row, rate_row * jnp.exp(total_row) * k_rate_row))
        inverses = [
            identity - jnp.where((row // 2) == (column // 2), lower, 0.0) for lower in lowers
        ]
        size = 2
        while size < span:
            joined = ((row // (2 * size)) == (column // (2 * size))) & (
                (row // size) != (column // size)
            )
            parts = [halves(inverse) for inverse in inverses]
            corner = [halves(jnp.where(joined, lower, 0.0)) for lower in lowers]
            first = [halves(dot3(p, c)) for p, c in zip(parts, corner)]
            inverses = [
                inverse - dot3(f, p) for inverse, f, p in zip(inverses, first, parts)
            ]
            size *= 2
        for (block, head), inverse, (value_rate, key_rate) in zip(chains, inverses, kept):
            columns = slice(head * head_dim, (head + 1) * head_dim)
            rows = pl.ds(pl.multiple_of(block * span, span), span)
            high, low = halves(inverse * value_rate)
            v_raw = v_ref[block, :, columns]
            base_ref[head, rows, :] = dot(high, v_raw) + dot(low, v_raw)
            high, low = halves(inverse * key_rate)
            k_raw = k_ref[block, :, columns]
            weight = halves(dot(high, k_raw) + dot(low, k_raw))
            weight_high[head, rows, :] = weight[0]
            weight_low[head, rows, :] = weight[1]
        return carry

    lax.fori_loop(0, blocks // together, prepare, 0)
    state_ref[...] = jnp.zeros_like(state_ref)
    gain = gain_ref[...]

    def advance(block, carry):
        rows = pl.ds(pl.multiple_of(block * span, span), span)
        for head in range(heads):
            columns = slice(head * head_dim, (head + 1) * head_dim)
            state = state_ref[head]
            parts = halves(state)
            scales = column_ref[head, rows, :]
            fresh = base_ref[head, rows, :] - dot3(
                (weight_high[head, rows, :], weight_low[head, rows, :]), parts
            )
            moved = halves(fresh * scales[:, 1:2])
            k_raw = k_ref[block, :, columns]
            q_raw = q_ref[block, :, columns]
            turned = (((0,), (0,)), ((), ()))
            gained = lax.dot_general(
                k_raw, moved[0], turned, preferred_element_type=jnp.float32
            ) + lax.dot_general(k_raw, moved[1], turned, preferred_element_type=jnp.float32)
            state_ref[head] = state * scales[:, 2:3] + gained
            output = (dot(q_raw, parts[0]) + dot(q_raw, parts[1])) * scales[:, 0:1] + dot(
                score_ref[head, rows, :], fresh.astype(jnp.bfloat16)
            )
            norm_scale = lax.rsqrt(jnp.mean(output * output, -1, keepdims=True) + 1e-05)
            out_ref[block, :, columns] = (output * norm_scale * gain).astype(jnp.bfloat16)
        return carry

    lax.fori_loop(0, blocks, advance, 0)


def recurrence(q_blocks, k_blocks, v_blocks, small, added, head_decay_rate, head_norm_gain):
    blocks, span, width = q_blocks.shape
    heads = head_decay_rate.shape[0]
    head_dim = width // heads
    vmem = pl.BlockSpec(memory_space=pltpu.VMEM)
    length = blocks * span
    return pl.pallas_call(
        recurrence_kernel,
        out_shape=jax.ShapeDtypeStruct(q_blocks.shape, jnp.bfloat16),
        in_specs=[vmem] * 5 + [pl.BlockSpec(memory_space=pltpu.SMEM), vmem],
        out_specs=vmem,
        scratch_shapes=[
            pltpu.VMEM((heads, length, head_dim), jnp.float32),
            pltpu.VMEM((heads, length, head_dim), jnp.bfloat16),
            pltpu.VMEM((heads, length, head_dim), jnp.bfloat16),
            pltpu.VMEM((heads, length, span), jnp.bfloat16),
            pltpu.VMEM((heads, length, head_dim), jnp.float32),
            pltpu.VMEM((heads, head_dim, head_dim), jnp.float32),
        ],
        cost_estimate=pl.CostEstimate(
            flops=heads * blocks * 40 * 2 * span * span * head_dim * 16,
            bytes_accessed=4 * length * width * 2,
            transcendentals=0,
        ),
    )(q_blocks, k_blocks, v_blocks, small, added, head_decay_rate, head_norm_gain[None, :])


def projection_pieces(weight):
    count = lax.axis_size("dp")
    pair = [(at, at ^ 1) for at in range(count)]
    me = lax.axis_index("dp")
    pieces = []
    for shift in range(0, count, 2):
        if shift == 0:
            moved = weight
        else:
            moved = lax.ppermute(
                weight, "dp", [(at, (at + shift) % count) for at in range(count)]
            )
        pieces.append((lax.rem(me - shift + count, count), moved))
        other = me + 1 - 2 * lax.rem(me, 2)
        pieces.append((lax.rem(other - shift + count, count), lax.ppermute(moved, "dp", pair)))
    return pieces


def layer_norm(values, gain):
    average = jnp.mean(values, -1, keepdims=True)
    centred = values - average
    variance = jnp.mean(centred * centred, -1, keepdims=True)
    return centred * lax.rsqrt(variance + 1e-05) * gain


def expert_rows(rows, gate_weight, up_weight, down_weight):
    flat_rows = rows.reshape(-1, rows.shape[-1])
    gate = jnp.minimum(
        jnp.dot(flat_rows, gate_weight, preferred_element_type=jnp.float32), CLAMP_LIMIT
    )
    upper = jnp.clip(
        jnp.dot(flat_rows, up_weight, preferred_element_type=jnp.float32), -CLAMP_LIMIT, CLAMP_LIMIT
    )
    hidden = (gate * jax.nn.sigmoid(SWISH_SLOPE * gate) * (upper + 1.0)).astype(jnp.bfloat16)
    produced = jnp.dot(hidden, down_weight, preferred_element_type=jnp.float32).astype(jnp.bfloat16)
    return produced.reshape(rows.shape)


def per_device(
    residual,
    query,
    key,
    value,
    output_gate_input,
    write_strength_logit,
    decay_head_input,
    added_log_decay,
    head_decay_rate,
    head_norm_gain,
    output_projection,
    mixer_norm_gain,
    token_expert_index,
    token_expert_weight,
    expert_gate_weight,
    expert_up_weight,
    expert_down_weight,
    feedforward_norm_gain,
):
    count = lax.axis_size("sp")
    tokens = query.shape[1]
    local_heads = head_decay_rate.shape[0]
    pieces = projection_pieces(output_projection)
    small = jnp.concatenate(
        [
            write_strength_logit[0].T.reshape(count, local_heads, tokens),
            decay_head_input[0].T.reshape(count, local_heads, tokens),
            jnp.zeros((count, 8 - 2 * local_heads, tokens), jnp.bfloat16),
        ],
        axis=1,
    ).astype(jnp.float32)
    q_blocks, k_blocks, v_blocks, small_blocks = spread_heads(
        (query, key, value, small), count
    )
    added = added_log_decay[0].reshape(local_heads, count, tokens).transpose(1, 0, 2)
    scaled = recurrence(
        q_blocks, k_blocks, v_blocks, small_blocks, added, head_decay_rate, head_norm_gain
    )
    returned = return_rows(scaled, count)
    token_rows = (
        returned.astype(jnp.float32) * jax.nn.silu(output_gate_input[0].astype(jnp.float32))
    ).astype(jnp.bfloat16)
    width = output_projection.shape[1]
    mixed = jnp.zeros((tokens, width * len(pieces)), jnp.float32)
    for owner, piece in pieces:
        mixed = lax.dynamic_update_slice(
            mixed,
            jnp.dot(token_rows, piece, preferred_element_type=jnp.float32),
            (0, owner * width),
        )
    normed = layer_norm(residual[0].astype(jnp.float32) + mixed, mixer_norm_gain).astype(
        jnp.bfloat16
    )
    experts = lax.axis_size("sp") * lax.axis_size("dp")
    tok_rows = normed.shape[0]
    picks = token_expert_index.shape[2]
    features = normed.shape[1]
    capacity = tok_rows * picks * 3 // (2 * experts)
    flat_ids = token_expert_index[0].reshape(-1)
    onehot = (flat_ids[:, None] == jnp.arange(experts, dtype=jnp.int32)[None, :]).astype(jnp.int32)
    earlier = jnp.cumsum(onehot, axis=0) - onehot
    slot_rank = jnp.sum(earlier * onehot, axis=1)
    destination = flat_ids * capacity + slot_rank
    source_token = (
        jnp.full((experts * capacity,), tok_rows, jnp.int32)
        .at[destination]
        .set(jnp.arange(tok_rows * picks, dtype=jnp.int32) // picks)
    )
    padded = jnp.concatenate([normed, jnp.zeros((1, features), jnp.bfloat16)], 0)
    dispatch = padded[source_token].reshape(experts, capacity, features)
    back = lax.all_to_all(
        expert_rows(
            lax.all_to_all(dispatch, ("sp", "dp"), split_axis=0, concat_axis=0, tiled=True),
            expert_gate_weight[0],
            expert_up_weight[0],
            expert_down_weight[0],
        ),
        ("sp", "dp"),
        split_axis=0,
        concat_axis=0,
        tiled=True,
    )
    results = back.reshape(experts * capacity, features)[destination].reshape(
        tok_rows, picks, features
    )
    weights = token_expert_weight[0]
    moe = jnp.zeros((tok_rows, features), jnp.float32)
    for pick in range(picks):
        moe = moe + weights[:, pick : pick + 1] * results[:, pick].astype(jnp.float32)
    return layer_norm(normed.astype(jnp.float32) + moe, feedforward_norm_gain)[None]


def solution(mesh):
    placed = (
        P("dp", "sp", None),
        P("dp", "sp", None),
        P("dp", "sp", None),
        P("dp", "sp", None),
        P("dp", "sp", None),
        P("dp", "sp", None),
        P("dp", "sp", None),
        P("dp", "sp", None),
        P("sp"),
        P(),
        P(None, "dp"),
        P(),
        P("dp", "sp", None),
        P("dp", "sp", None),
        P(("sp", "dp"), None, None),
        P(("sp", "dp"), None, None),
        P(("sp", "dp"), None, None),
        P(),
    )
    return jax.shard_map(
        per_device, mesh=mesh, in_specs=placed, out_specs=P("dp", "sp", None), check_vma=False
    )
```

```python
import functools

import jax
import jax.numpy as jnp
from jax import lax
from jax.experimental import pallas as pl
from jax.experimental.pallas import tpu as pltpu
from jax.sharding import PartitionSpec as P

CLAMP_LIMIT = 7.0
SWISH_SLOPE = 1.702
MESH = pl.DeviceIdType.MESH


def greet_peers(count):
    me = lax.axis_index("sp")
    barrier = pltpu.get_barrier_semaphore()
    for offset in range(1, count):
        pl.semaphore_signal(
            barrier, inc=1, device_id={"sp": lax.rem(me + offset, count)}, device_id_type=MESH
        )
    pl.semaphore_wait(barrier, count - 1)


def spread_heads_kernel(count, *refs):
    arrays = (len(refs) - 3) // 2
    sources, targets = refs[:arrays], refs[arrays : 2 * arrays]
    send_sem, recv_sem, local_sem = refs[2 * arrays :]
    me = lax.axis_index("sp")

    def piece(source, owner):
        if source.shape[0] == count:
            return source.at[owner]
        width = source.shape[2] // count
        return source.at[0, :, pl.ds(pl.multiple_of(owner * width, width), width)]

    def place(target, owner):
        return target.at[owner]

    greet_peers(count)
    copies = []
    for offset in range(1, count):
        peer = lax.rem(me + offset, count)
        for at in range(arrays):
            copy = pltpu.make_async_remote_copy(
                src_ref=piece(sources[at], peer),
                dst_ref=place(targets[at], me),
                send_sem=send_sem.at[at, offset],
                recv_sem=recv_sem.at[at, offset],
                device_id={"sp": peer},
                device_id_type=MESH,
            )
            copy.start()
            copies.append(copy)
    for at in range(arrays):
        copy = pltpu.make_async_copy(
            piece(sources[at], me), place(targets[at], me), local_sem.at[at]
        )
        copy.start()
        copies.append(copy)
    for copy in copies:
        copy.wait()


def spread_heads(sources, count):
    shapes = []
    for source in sources:
        if source.shape[0] == count:
            shapes.append(jax.ShapeDtypeStruct(source.shape, source.dtype))
        else:
            shapes.append(
                jax.ShapeDtypeStruct(
                    (count, source.shape[1], source.shape[2] // count), source.dtype
                )
            )
    return pl.pallas_call(
        functools.partial(spread_heads_kernel, count),
        out_shape=shapes,
        in_specs=[pl.BlockSpec(memory_space=pltpu.VMEM)] * len(sources),
        out_specs=[pl.BlockSpec(memory_space=pl.ANY)] * len(sources),
        scratch_shapes=[
            pltpu.SemaphoreType.DMA((len(sources), count)),
            pltpu.SemaphoreType.DMA((len(sources), count)),
            pltpu.SemaphoreType.DMA((len(sources),)),
        ],
        compiler_params=pltpu.CompilerParams(collective_id=0, has_side_effects=True),
    )(*sources)


def return_rows_kernel(count, source, target, send_sem, recv_sem, local_sem):
    me = lax.axis_index("sp")
    width = source.shape[2]
    own_columns = pl.ds(pl.multiple_of(me * width, width), width)
    greet_peers(count)
    copies = []
    for offset in range(1, count):
        peer = lax.rem(me + offset, count)
        copy = pltpu.make_async_remote_copy(
            src_ref=source.at[peer],
            dst_ref=target.at[:, own_columns],
            send_sem=send_sem.at[offset],
            recv_sem=recv_sem.at[offset],
            device_id={"sp": peer},
            device_id_type=MESH,
        )
        copy.start()
        copies.append(copy)
    copy = pltpu.make_async_copy(source.at[me], target.at[:, own_columns], local_sem)
    copy.start()
    copies.append(copy)
    for copy in copies:
        copy.wait()


def return_rows(source, count):
    return pl.pallas_call(
        functools.partial(return_rows_kernel, count),
        out_shape=jax.ShapeDtypeStruct(
            (source.shape[1], source.shape[2] * count), source.dtype
        ),
        in_specs=[pl.BlockSpec(memory_space=pltpu.VMEM)],
        out_specs=pl.BlockSpec(memory_space=pltpu.VMEM),
        scratch_shapes=[
            pltpu.SemaphoreType.DMA((count,)),
            pltpu.SemaphoreType.DMA((count,)),
            pltpu.SemaphoreType.DMA,
        ],
        compiler_params=pltpu.CompilerParams(collective_id=1, has_side_effects=True),
    )(source)


def dot(left, right):
    return jnp.dot(left, right, preferred_element_type=jnp.float32)


def halves(values):
    high = values.astype(jnp.bfloat16)
    return high, (values - high.astype(jnp.float32)).astype(jnp.bfloat16)


def dot3(left, right):
    return dot(left[0], right[0]) + (dot(left[0], right[1]) + dot(left[1], right[0]))


def rows_by_rows(left, right):
    return lax.dot_general(
        left, right, (((1,), (1,)), ((), ())), preferred_element_type=jnp.float32
    )


def recurrence_kernel(
    q_ref, k_ref, v_ref, small_ref, added_ref, decay_ref, gain_ref, out_ref,
    base_ref, weight_high, weight_low, score_ref, column_ref, state_ref,
):
    blocks, span, width = q_ref.shape
    heads = added_ref.shape[1]
    head_dim = width // heads
    row = lax.broadcasted_iota(jnp.int32, (span, span), 0)
    column = lax.broadcasted_iota(jnp.int32, (span, span), 1)
    same = row == column
    inclusive = row >= column
    strict = row > column
    identity = same.astype(jnp.float32)

    def to_column(values):
        return jnp.sum(jnp.where(same, values, 0.0), axis=1, keepdims=True)

    def to_row(values):
        return jnp.sum(jnp.where(same, values, 0.0), axis=0, keepdims=True)

    lanes = lax.broadcasted_iota(jnp.int32, (span, head_dim), 1)
    together = 2 if blocks % 2 == 0 else 1

    def prepare(step, carry):
        chains = [(step * together + i, h) for i in range(together) for h in range(heads)]
        lowers = []
        kept = []
        for block, head in chains:
            columns = slice(head * head_dim, (head + 1) * head_dim)
            q_raw = q_ref[block, :, columns]
            k_raw = k_ref[block, :, columns]
            q_wide = q_raw.astype(jnp.float32)
            q_rate = (
                lax.rsqrt(jnp.sum(q_wide * q_wide, 1, keepdims=True) + 1e-06)
                * head_dim ** (-0.5)
            )
            k_dot = rows_by_rows(k_raw, k_raw)
            k_wide = k_raw.astype(jnp.float32)
            k_rate = lax.rsqrt(jnp.sum(k_wide * k_wide, 1, keepdims=True) + 1e-06)
            k_rate_row = to_row(k_rate)
            rate_row = jax.nn.sigmoid(small_ref[block, head : head + 1, :])
            sequence_row = small_ref[block, heads + head : heads + head + 1, :]
            softplus = jnp.maximum(sequence_row, 0.0) + jnp.log1p(
                jnp.exp(-jnp.abs(sequence_row))
            )
            log_decay = (
                added_ref[block, head : head + 1, :] - decay_ref[head] * softplus
            )
            total = jnp.sum(jnp.where(inclusive, log_decay, 0.0), axis=1, keepdims=True)
            total_row = to_row(total)
            last = total[span - 1 : span, :]
            within = jnp.exp(jnp.where(inclusive, total - total_row, -1e30))
            lower = jnp.where(
                strict, to_column(rate_row) * within * k_dot * (k_rate * k_rate_row), 0.0
            )
            scores = rows_by_rows(q_raw, k_raw) * within * (q_rate * k_rate_row)
            rows = pl.ds(pl.multiple_of(block * span, span), span)
            score_ref[head, rows, :] = scores.astype(jnp.bfloat16)
            column_ref[head, rows, :] = jnp.where(
                lanes == 0,
                q_rate * jnp.exp(total),
                jnp.where(lanes == 1, k_rate * jnp.exp(last - total), jnp.exp(last)),
            )
            lowers.append(lower)
            kept.append((rate_row, rate_row * jnp.exp(total_row) * k_rate_row))
        inverses = [
            identity - jnp.where((row // 2) == (column // 2), lower, 0.0) for lower in lowers
        ]
        size = 2
        while size < span:
            joined = ((row // (2 * size)) == (column // (2 * size))) & (
                (row // size) != (column // size)
            )
            parts = [halves(inverse) for inverse in inverses]
            corner = [halves(jnp.where(joined, lower, 0.0)) for lower in lowers]
            first = [halves(dot3(p, c)) for p, c in zip(parts, corner)]
            inverses = [
                inverse - dot3(f, p) for inverse, f, p in zip(inverses, first, parts)
            ]
            size *= 2
        for (block, head), inverse, (value_rate, key_rate) in zip(chains, inverses, kept):
            columns = slice(head * head_dim, (head + 1) * head_dim)
            rows = pl.ds(pl.multiple_of(block * span, span), span)
            high, low = halves(inverse * value_rate)
            v_raw = v_ref[block, :, columns]
            base_ref[head, rows, :] = dot(high, v_raw) + dot(low, v_raw)
            high, low = halves(inverse * key_rate)
            k_raw = k_ref[block, :, columns]
            weight = halves(dot(high, k_raw) + dot(low, k_raw))
            weight_high[head, rows, :] = weight[0]
            weight_low[head, rows, :] = weight[1]
        return carry

    lax.fori_loop(0, blocks // together, prepare, 0)
    state_ref[...] = jnp.zeros_like(state_ref)
    gain = gain_ref[...]

    def advance(block, carry):
        rows = pl.ds(pl.multiple_of(block * span, span), span)
        for head in range(heads):
            columns = slice(head * head_dim, (head + 1) * head_dim)
            state = state_ref[head]
            parts = halves(state)
            scales = column_ref[head, rows, :]
            fresh = base_ref[head, rows, :] - dot3(
                (weight_high[head, rows, :], weight_low[head, rows, :]), parts
            )
            moved = halves(fresh * scales[:, 1:2])
            k_raw = k_ref[block, :, columns]
            q_raw = q_ref[block, :, columns]
            turned = (((0,), (0,)), ((), ()))
            gained = lax.dot_general(
                k_raw, moved[0], turned, preferred_element_type=jnp.float32
            ) + lax.dot_general(k_raw, moved[1], turned, preferred_element_type=jnp.float32)
            state_ref[head] = state * scales[:, 2:3] + gained
            output = (dot(q_raw, parts[0]) + dot(q_raw, parts[1])) * scales[:, 0:1] + dot(
                score_ref[head, rows, :], fresh.astype(jnp.bfloat16)
            )
            norm_scale = lax.rsqrt(jnp.mean(output * output, -1, keepdims=True) + 1e-05)
            out_ref[block, :, columns] = (output * norm_scale * gain).astype(jnp.bfloat16)
        return carry

    lax.fori_loop(0, blocks, advance, 0)


def recurrence(q_blocks, k_blocks, v_blocks, small, added, head_decay_rate, head_norm_gain):
    blocks, span, width = q_blocks.shape
    heads = head_decay_rate.shape[0]
    head_dim = width // heads
    vmem = pl.BlockSpec(memory_space=pltpu.VMEM)
    length = blocks * span
    return pl.pallas_call(
        recurrence_kernel,
        out_shape=jax.ShapeDtypeStruct(q_blocks.shape, jnp.bfloat16),
        in_specs=[vmem] * 5 + [pl.BlockSpec(memory_space=pltpu.SMEM), vmem],
        out_specs=vmem,
        scratch_shapes=[
            pltpu.VMEM((heads, length, head_dim), jnp.float32),
            pltpu.VMEM((heads, length, head_dim), jnp.bfloat16),
            pltpu.VMEM((heads, length, head_dim), jnp.bfloat16),
            pltpu.VMEM((heads, length, span), jnp.bfloat16),
            pltpu.VMEM((heads, length, head_dim), jnp.float32),
            pltpu.VMEM((heads, head_dim, head_dim), jnp.float32),
        ],
        cost_estimate=pl.CostEstimate(
            flops=heads * blocks * 40 * 2 * span * span * head_dim * 16,
            bytes_accessed=4 * length * width * 2,
            transcendentals=0,
        ),
    )(q_blocks, k_blocks, v_blocks, small, added, head_decay_rate, head_norm_gain[None, :])


def projection_pieces(weight):
    count = lax.axis_size("dp")
    pair = [(at, at ^ 1) for at in range(count)]
    me = lax.axis_index("dp")
    pieces = []
    for shift in range(0, count, 2):
        if shift == 0:
            moved = weight
        else:
            moved = lax.ppermute(
                weight, "dp", [(at, (at + shift) % count) for at in range(count)]
            )
        pieces.append((lax.rem(me - shift + count, count), moved))
        other = me + 1 - 2 * lax.rem(me, 2)
        pieces.append((lax.rem(other - shift + count, count), lax.ppermute(moved, "dp", pair)))
    return pieces


def plane_split(count):
    across = 1 << ((count.bit_length() - 1) // 2)
    return count // across, across


def dispatch_kernel(
    layers, across, cores, rows_ref, pick_ref, out_ref, held, staged,
    row_send, row_recv, out_send, out_recv, local_sem,
):
    experts = across * cores
    place = lax.axis_index("sp")
    core = lax.axis_index("dp")
    layer = lax.div(place, across)
    column = lax.rem(place, across)
    member = column * cores + core
    capacity = staged.shape[2]
    features = rows_ref.shape[1]
    tile = features // 4

    def peer_at(offset):
        other = lax.rem(member + offset, experts)
        where = {"sp": layer * across + lax.div(other, cores), "dp": lax.rem(other, cores)}
        return other, where

    def row_copy(source, slot, way):
        step = 1 - 2 * way
        return pltpu.make_async_remote_copy(
            src_ref=source,
            dst_ref=held.at[slot],
            send_sem=row_send.at[way, slot],
            recv_sem=row_recv.at[slot],
            device_id={"sp": lax.rem(place + step * across + layers * across, layers * across)},
            device_id_type=MESH,
        )

    def out_copy(slot, offset):
        other, where = peer_at(offset)
        return pltpu.make_async_remote_copy(
            src_ref=staged.at[slot, other],
            dst_ref=out_ref.at[slot * experts + member],
            send_sem=out_send.at[slot, offset],
            recv_sem=out_recv.at[slot, offset],
            device_id=where,
            device_id_type=MESH,
        )

    def own_copy(slot):
        return pltpu.make_async_copy(
            staged.at[slot, member], out_ref.at[slot * experts + member], local_sem.at[slot]
        )

    barrier = pltpu.get_barrier_semaphore()
    for offset in range(1, experts):
        pl.semaphore_signal(
            barrier, inc=1, device_id=peer_at(offset)[1], device_id_type=MESH
        )

    @pl.when(layer > 0)
    def _():
        pl.semaphore_signal(
            barrier, inc=1, device_id={"sp": place - across}, device_id_type=MESH
        )

    @pl.when(layer < layers - 1)
    def _():
        pl.semaphore_signal(
            barrier, inc=1, device_id={"sp": place + across}, device_id_type=MESH
        )

    inner = (layer > 0) & (layer < layers - 1)

    @pl.when(inner)
    def _():
        pl.semaphore_wait(barrier, experts + 1)

    @pl.when(jnp.logical_not(inner))
    def _():
        pl.semaphore_wait(barrier, experts if layers > 1 else experts - 1)

    def serve(slot, source):
        picks = pick_ref[slot]
        for at in range(4):
            columns = slice(at * tile, (at + 1) * tile)
            chosen = jnp.dot(picks, source[:, columns], preferred_element_type=jnp.float32)
            staged[slot, :, :, columns] = chosen.reshape(experts, capacity, tile).astype(
                jnp.bfloat16
            )
        for offset in range(1, experts):
            out_copy(slot, offset).start()
        own_copy(slot).start()

    @pl.when(layer < layers - 1)
    def _():
        row_copy(rows_ref, layer, 0).start()

    @pl.when(layer > 0)
    def _():
        row_copy(rows_ref, layer, 1).start()

    serve(layer, rows_ref)
    for distance in range(1, layers):
        for way in range(2):
            slot = layer - distance if way == 0 else layer + distance
            here = slot >= 0 if way == 0 else slot < layers
            onward = layer < layers - 1 if way == 0 else layer > 0

            @pl.when(here)
            def _(slot=slot, way=way, onward=onward):
                row_copy(rows_ref, slot, way).wait_recv()

                @pl.when(onward)
                def _():
                    row_copy(held.at[slot], slot, way).start()

                serve(slot, held.at[slot])

    for slot in range(layers):

        @pl.when((layer < layers - 1) & (slot <= layer))
        def _(slot=slot):
            row_copy(rows_ref, slot, 0).wait_send()

        @pl.when((layer > 0) & (slot >= layer))
        def _(slot=slot):
            row_copy(rows_ref, slot, 1).wait_send()

        for offset in range(1, experts):
            out_copy(slot, offset).wait()
        own_copy(slot).wait()


def dispatch_rows(rows, picks, capacity):
    count, cores = lax.axis_size("sp"), lax.axis_size("dp")
    layers, across = plane_split(count)
    experts = across * cores
    tokens, features = rows.shape
    vmem = pl.BlockSpec(memory_space=pltpu.VMEM)
    return pl.pallas_call(
        functools.partial(dispatch_kernel, layers, across, cores),
        out_shape=jax.ShapeDtypeStruct((layers * experts, capacity, features), rows.dtype),
        in_specs=[vmem, vmem],
        out_specs=pl.BlockSpec(memory_space=pl.ANY),
        scratch_shapes=[
            pltpu.VMEM((layers, tokens, features), rows.dtype),
            pltpu.VMEM((layers, experts, capacity, features), rows.dtype),
            pltpu.SemaphoreType.DMA((2, layers)),
            pltpu.SemaphoreType.DMA((layers,)),
            pltpu.SemaphoreType.DMA((layers, experts)),
            pltpu.SemaphoreType.DMA((layers, experts)),
            pltpu.SemaphoreType.DMA((layers,)),
        ],
        compiler_params=pltpu.CompilerParams(collective_id=2, has_side_effects=True),
    )(rows, picks)


def combine_kernel(
    layers, across, cores, rows_ref, high_ref, low_ref, out_ref, back, arrived, leaving,
    back_send, back_recv, sum_send, sum_recv, local_sem,
):
    experts = across * cores
    place = lax.axis_index("sp")
    core = lax.axis_index("dp")
    layer = lax.div(place, across)
    column = lax.rem(place, across)
    member = column * cores + core
    capacity, features = back.shape[2:]
    tile = features // 4

    def peer_at(offset):
        other = lax.rem(member + offset, experts)
        where = {"sp": layer * across + lax.div(other, cores), "dp": lax.rem(other, cores)}
        return other, where

    def back_copy(slot, offset):
        other, where = peer_at(offset)
        return pltpu.make_async_remote_copy(
            src_ref=rows_ref.at[slot * experts + other],
            dst_ref=back.at[slot, member],
            send_sem=back_send.at[slot, offset],
            recv_sem=back_recv.at[slot, offset],
            device_id=where,
            device_id_type=MESH,
        )

    def own_copy(slot):
        return pltpu.make_async_copy(
            rows_ref.at[slot * experts + member], back.at[slot, member], local_sem.at[slot]
        )

    def sum_copy(slot, way):
        step = 1 - 2 * way
        return pltpu.make_async_remote_copy(
            src_ref=leaving.at[slot],
            dst_ref=arrived.at[way, slot],
            send_sem=sum_send.at[slot],
            recv_sem=sum_recv.at[way, slot],
            device_id={"sp": lax.rem(place + step * across + layers * across, layers * across)},
            device_id_type=MESH,
        )

    barrier = pltpu.get_barrier_semaphore()
    for offset in range(1, experts):
        pl.semaphore_signal(
            barrier, inc=1, device_id=peer_at(offset)[1], device_id_type=MESH
        )

    @pl.when(layer > 0)
    def _():
        pl.semaphore_signal(
            barrier, inc=1, device_id={"sp": place - across}, device_id_type=MESH
        )

    @pl.when(layer < layers - 1)
    def _():
        pl.semaphore_signal(
            barrier, inc=1, device_id={"sp": place + across}, device_id_type=MESH
        )

    inner = (layer > 0) & (layer < layers - 1)

    @pl.when(inner)
    def _():
        pl.semaphore_wait(barrier, experts + 1)

    @pl.when(jnp.logical_not(inner))
    def _():
        pl.semaphore_wait(barrier, experts if layers > 1 else experts - 1)

    def send_back(slot):
        for offset in range(1, experts):
            back_copy(slot, offset).start()
        own_copy(slot).start()

    def partial_sum(slot, columns):
        produced = (
            back[slot, :, :, columns]
            .astype(jnp.float32)
            .reshape(experts * capacity, tile)
            .astype(jnp.bfloat16)
        )
        turned = (((0,), (0,)), ((), ()))
        return lax.dot_general(
            high_ref[slot], produced, turned, preferred_element_type=jnp.float32
        ) + lax.dot_general(
            low_ref[slot], produced, turned, preferred_element_type=jnp.float32
        )

    def gather_back(slot):
        for offset in range(1, experts):
            back_copy(slot, offset).wait()
        own_copy(slot).wait()

    for distance in range(layers - 1, 0, -1):
        for way in range(2):
            slot = layer + distance if way == 0 else layer - distance

            @pl.when((slot < layers) if way == 0 else (slot >= 0))
            def _(slot=slot):
                send_back(slot)

    send_back(layer)

    for distance in range(layers - 1, 0, -1):
        for way in range(2):
            slot = layer + distance if way == 0 else layer - distance
            upstream = layer > 0 if way == 0 else layer < layers - 1

            @pl.when((slot < layers) if way == 0 else (slot >= 0))
            def _(slot=slot, way=way, upstream=upstream):
                gather_back(slot)

                @pl.when(upstream)
                def _():
                    sum_copy(slot, way).wait_recv()
                    for at in range(4):
                        columns = slice(at * tile, (at + 1) * tile)
                        leaving[slot, :, columns] = (
                            partial_sum(slot, columns)
                            + arrived[way, slot, :, columns].astype(jnp.float32)
                        ).astype(jnp.bfloat16)

                @pl.when(jnp.logical_not(upstream))
                def _():
                    for at in range(4):
                        columns = slice(at * tile, (at + 1) * tile)
                        leaving[slot, :, columns] = partial_sum(slot, columns).astype(
                            jnp.bfloat16
                        )

                sum_copy(slot, way).start()

    gather_back(layer)
    for at in range(4):
        columns = slice(at * tile, (at + 1) * tile)
        out_ref[:, columns] = partial_sum(layer, columns)

    for way in range(2):

        @pl.when((layer > 0) if way == 0 else (layer < layers - 1))
        def _(way=way):
            sum_copy(layer, way).wait_recv()
            out_ref[...] += arrived[way, layer].astype(jnp.float32)

    for distance in range(1, layers):
        for way in range(2):
            slot = layer + distance if way == 0 else layer - distance

            @pl.when((slot < layers) if way == 0 else (slot >= 0))
            def _(slot=slot, way=way):
                sum_copy(slot, way).wait_send()


def combine_rows(produced, high, low):
    count, cores = lax.axis_size("sp"), lax.axis_size("dp")
    layers, across = plane_split(count)
    experts = across * cores
    capacity, features = produced.shape[1:]
    tokens = high.shape[2]
    vmem = pl.BlockSpec(memory_space=pltpu.VMEM)
    return pl.pallas_call(
        functools.partial(combine_kernel, layers, across, cores),
        out_shape=jax.ShapeDtypeStruct((tokens, features), jnp.float32),
        in_specs=[pl.BlockSpec(memory_space=pl.ANY), vmem, vmem],
        out_specs=vmem,
        scratch_shapes=[
            pltpu.VMEM((layers, experts, capacity, features), produced.dtype),
            pltpu.VMEM((2, layers, tokens, features), produced.dtype),
            pltpu.VMEM((layers, tokens, features), produced.dtype),
            pltpu.SemaphoreType.DMA((layers, experts)),
            pltpu.SemaphoreType.DMA((layers, experts)),
            pltpu.SemaphoreType.DMA((layers,)),
            pltpu.SemaphoreType.DMA((2, layers)),
            pltpu.SemaphoreType.DMA((layers,)),
        ],
        compiler_params=pltpu.CompilerParams(collective_id=3, has_side_effects=True),
    )(produced, high, low)


def plane_picks(ids, weights, capacity):
    count, cores = lax.axis_size("sp"), lax.axis_size("dp")
    layers, across = plane_split(count)
    experts = across * cores
    place = lax.axis_index("sp")
    picks, tokens = ids.shape[1:]
    ids = lax.dynamic_index_in_dim(
        ids.reshape(layers, across, picks, tokens), lax.rem(place, across), 1, keepdims=False
    )
    mine = (lax.div(place, across) * experts + jnp.arange(experts)).astype(jnp.float32)
    weights = lax.dynamic_index_in_dim(
        weights.reshape(layers, across, picks, tokens), lax.rem(place, across), 1, keepdims=False
    )
    matches = ids[:, None] == mine[None, :, None, None]
    named = jnp.any(matches, axis=2)
    share = jnp.sum(jnp.where(matches, weights[:, None], 0.0), axis=2)[:, :, None, :]
    order = jnp.arange(tokens)
    before = (order[:, None] < order[None, :]).astype(jnp.bfloat16)
    rank = jnp.dot(
        named.astype(jnp.bfloat16).reshape(layers * experts, tokens),
        before,
        preferred_element_type=jnp.float32,
    ).reshape(layers, experts, 1, tokens)
    slots = jnp.arange(capacity, dtype=jnp.float32)[None, None, :, None]
    chosen = named[:, :, None, :] & (rank == slots)
    shape = (layers, experts * capacity, tokens)
    share_high, share_low = halves(share)
    none = jnp.zeros((), jnp.bfloat16)
    return (
        chosen.astype(jnp.bfloat16).reshape(shape),
        jnp.where(chosen, share_high, none).reshape(shape),
        jnp.where(chosen, share_low, none).reshape(shape),
    )


def layer_norm(values, gain):
    average = jnp.mean(values, -1, keepdims=True)
    centred = values - average
    variance = jnp.mean(centred * centred, -1, keepdims=True)
    return centred * lax.rsqrt(variance + 1e-05) * gain


def expert_rows(rows, gate_weight, up_weight, down_weight):
    flat_rows = rows.reshape(-1, rows.shape[-1])
    gate = jnp.minimum(
        jnp.dot(flat_rows, gate_weight, preferred_element_type=jnp.float32), CLAMP_LIMIT
    )
    upper = jnp.clip(
        jnp.dot(flat_rows, up_weight, preferred_element_type=jnp.float32), -CLAMP_LIMIT, CLAMP_LIMIT
    )
    hidden = (gate * jax.nn.sigmoid(SWISH_SLOPE * gate) * (upper + 1.0)).astype(jnp.bfloat16)
    produced = jnp.dot(hidden, down_weight, preferred_element_type=jnp.float32).astype(jnp.bfloat16)
    return produced.reshape(rows.shape)


def per_device(
    residual,
    query,
    key,
    value,
    output_gate_input,
    write_strength_logit,
    decay_head_input,
    added_log_decay,
    head_decay_rate,
    head_norm_gain,
    output_projection,
    mixer_norm_gain,
    token_expert_index,
    token_expert_weight,
    expert_gate_weight,
    expert_up_weight,
    expert_down_weight,
    feedforward_norm_gain,
):
    count = lax.axis_size("sp")
    tokens = query.shape[1]
    local_heads = head_decay_rate.shape[0]
    pieces = projection_pieces(output_projection)
    picks = token_expert_index.shape[2]
    spare = -(2 * local_heads + 2 * picks) % 8
    small = jnp.concatenate(
        [
            write_strength_logit[0].T.reshape(count, local_heads, tokens).astype(jnp.float32),
            decay_head_input[0].T.reshape(count, local_heads, tokens).astype(jnp.float32),
            jnp.broadcast_to(
                token_expert_index[0].T.astype(jnp.float32)[None], (count, picks, tokens)
            ),
            jnp.broadcast_to(token_expert_weight[0].T[None], (count, picks, tokens)),
            jnp.zeros((count, spare, tokens), jnp.float32),
        ],
        axis=1,
    )
    q_blocks, k_blocks, v_blocks, small_blocks = spread_heads(
        (query, key, value, small), count
    )
    experts = count * lax.axis_size("dp")
    capacity = tokens * picks * 3 // (2 * experts)
    first = 2 * local_heads
    chosen, share_high, share_low = plane_picks(
        small_blocks[:, first : first + picks],
        small_blocks[:, first + picks : first + 2 * picks],
        capacity,
    )
    added = added_log_decay[0].reshape(local_heads, count, tokens).transpose(1, 0, 2)
    scaled = recurrence(
        q_blocks, k_blocks, v_blocks, small_blocks, added, head_decay_rate, head_norm_gain
    )
    returned = return_rows(scaled, count)
    token_rows = (
        returned.astype(jnp.float32) * jax.nn.silu(output_gate_input[0].astype(jnp.float32))
    ).astype(jnp.bfloat16)
    width = output_projection.shape[1]
    mixed = jnp.zeros((tokens, width * len(pieces)), jnp.float32)
    for owner, piece in pieces:
        mixed = lax.dynamic_update_slice(
            mixed,
            jnp.dot(token_rows, piece, preferred_element_type=jnp.float32),
            (0, owner * width),
        )
    normed = layer_norm(residual[0].astype(jnp.float32) + mixed, mixer_norm_gain).astype(
        jnp.bfloat16
    )
    produced = expert_rows(
        dispatch_rows(normed, chosen, capacity),
        expert_gate_weight[0],
        expert_up_weight[0],
        expert_down_weight[0],
    )
    moe = combine_rows(produced, share_high, share_low)
    return layer_norm(normed.astype(jnp.float32) + moe, feedforward_norm_gain)[None]


def solution(mesh):
    placed = (
        P("dp", "sp", None),
        P("dp", "sp", None),
        P("dp", "sp", None),
        P("dp", "sp", None),
        P("dp", "sp", None),
        P("dp", "sp", None),
        P("dp", "sp", None),
        P("dp", "sp", None),
        P("sp"),
        P(),
        P(None, "dp"),
        P(),
        P("dp", "sp", None),
        P("dp", "sp", None),
        P(("sp", "dp"), None, None),
        P(("sp", "dp"), None, None),
        P(("sp", "dp"), None, None),
        P(),
    )
    return jax.shard_map(
        per_device, mesh=mesh, in_specs=placed, out_specs=P("dp", "sp", None), check_vma=False
    )
```
